32 devices in a mesh: sp: 8 (over z, y), tp: 4 (over x, core).
Axes of the slice: x: 2, y: 2, z: 4, core: 2. Of those that a mesh axis runs over, the one named last changes fastest.
Arguments:
- residual: bfloat16 [5120, 2048], P('sp', 'tp'), may hold values from -4 to 4
- query_wide: bfloat16 [5120, 1536], P('sp', 'tp'), may hold values from -500 to 500
- query_narrow: bfloat16 [5120, 1024], P('sp', 'tp'), may hold values from -500 to 500
- latent: bfloat16 [5120, 512], P('sp'), may hold values from -6 to 6
- rope_key: bfloat16 [5120, 64], P('sp'), may hold values from -6 to 6
- latent_gain: float32 [512], replicated, may hold values from 0.1 to 1.9
- expand_wide: bfloat16 [512, 2048], P(None, 'tp'), may hold values from -0.25 to 0.25
- expand_narrow: bfloat16 [512, 1024], P(None, 'tp'), may hold values from -0.25 to 0.25
- out_wide: bfloat16 [1024, 2048], P('tp'), may hold values from -0.1875 to 0.1875
- out_narrow: bfloat16 [512, 2048], P('tp'), may hold values from -0.25 to 0.25
- norm_gain: float32 [2048], P('tp'), may hold values from 0.1 to 1.9
- up_gate: bfloat16 [2048, 5632], P('sp', 'tp'), may hold values from -0.125 to 0.125
- up_value: bfloat16 [2048, 5632], P('sp', 'tp'), may hold values from -0.125 to 0.125
- down_weight: bfloat16 [2048, 5632], P('sp', 'tp'), may hold values from -0.078125 to 0.078125
- conv_taps: float32 [3, 2, 5632], P(None, None, 'tp'), may hold values from -3 to 3
Outputs:
- output: bfloat16 [5120, 2048], P('sp', 'tp')
The draws below stay inside these ranges and needn't reach their ends.
All inputs are finite; a program needn't handle non-finite values.
Results may differ from the reference program's by a relative error of at most 0.025.
Values may be sent and summed in bfloat16 or wider, within the bound.
A program may use at most 192 MiB of HBM per device.

```python
import math
import jax
import jax.numpy as jnp
from jax import lax

D = 2048
FF = 5632
RANK = 512
ROPE = 64
HW = 8
NOPE_W = 128
VAL_W = 128
HN = 8
NOPE_N = 64
VAL_N = 64
TOKENS = 5120
N_TP = 4


def draw_residual(key, part):
    key_noise = jax.random.fold_in(key, 11)
    columns = jnp.arange(D, dtype=jnp.float32) / D
    values = jax.random.normal(key_noise, (TOKENS, D), jnp.float32) * 0.1 * jnp.exp(1.6 * columns)[None, :]
    return jnp.clip(values, -4.0, 4.0).astype(jnp.bfloat16)


def query_values(key, arr_shape):
    key_noise = jax.random.fold_in(key, 21)
    values = jax.random.normal(key_noise, arr_shape, jnp.float32) * 2.5
    return jnp.clip(values, -12.0, 12.0)


def draw_query_wide(key, part):
    return query_values(jax.random.fold_in(key, 1), (TOKENS, HW * (NOPE_W + ROPE))).astype(jnp.bfloat16)


def draw_query_narrow(key, part):
    return query_values(jax.random.fold_in(key, 2), (TOKENS, HN * (NOPE_N + ROPE))).astype(jnp.bfloat16)


def level_of(key, dims, cuts, smallest, high):
    gain = 1.0
    for dim, blocks in cuts:
        draws = jax.random.uniform(jax.random.fold_in(jax.random.fold_in(key, 6), dim), (blocks,), jnp.float32, smallest / len(cuts), high / len(cuts))
        gain = gain * jnp.repeat(jnp.exp(draws), dims[dim] // blocks).reshape((-1,) + (1,) * (len(dims) - 1 - dim))
    return gain


def scatter_about(key, extent, scale, reach, cuts=(), kind=jnp.bfloat16):
    level = level_of(key, extent, cuts, -0.22, 0.18) if cuts else 1.0
    values = jax.random.normal(key, extent, jnp.float32) * scale * level
    return jnp.minimum(jnp.maximum(values, -reach), reach).astype(kind)


def setup_inputs(seed: int = 0) -> dict:
    arg_keys = jax.random.split(jax.random.key(seed), 16)
    return {
        "residual": draw_residual(jax.random.fold_in(arg_keys[15], 71), 0),
        "query_wide": draw_query_wide(jax.random.fold_in(arg_keys[15], 71), 0),
        "query_narrow": draw_query_narrow(jax.random.fold_in(arg_keys[15], 71), 0),
        "latent": scatter_about(arg_keys[3], (TOKENS, RANK), 1.0, 6.0, ((0, 8),)),
        "rope_key": scatter_about(arg_keys[4], (TOKENS, ROPE), 1.0, 6.0, ((0, 8),)),
        "latent_gain": jnp.clip(1.0 + 0.18 * jax.random.normal(arg_keys[5], (RANK,), jnp.float32), 0.1, 1.9),
        "expand_wide": scatter_about(arg_keys[6], (RANK, HW * (NOPE_W + VAL_W)), RANK ** -0.5, 0.25, ((1, 4),)),
        "expand_narrow": scatter_about(arg_keys[7], (RANK, HN * (NOPE_N + VAL_N)), RANK ** -0.5, 0.25, ((1, 4),)),
        "out_wide": scatter_about(arg_keys[8], (HW * VAL_W, D), (HW * VAL_W) ** -0.5, 0.1875, ((0, 4),)),
        "out_narrow": scatter_about(arg_keys[9], (HN * VAL_N, D), (HN * VAL_N) ** -0.5, 0.25, ((0, 4),)),
        "norm_gain": jnp.clip(1.0 + 0.18 * jax.random.normal(arg_keys[10], (D,), jnp.float32), 0.1, 1.9),
        "up_gate": scatter_about(arg_keys[11], (D, FF), D ** -0.5, 0.125, ((0, 8), (1, 4))),
        "up_value": scatter_about(arg_keys[12], (D, FF), D ** -0.5, 0.125, ((0, 8), (1, 4))),
        "down_weight": scatter_about(arg_keys[13], (D, FF), FF ** -0.5, 0.078125, ((0, 8), (1, 4))),
        "conv_taps": scatter_about(arg_keys[14], (3, 2, FF), 0.6, 3.0, ((2, 4),), jnp.float32),
    }


theta = 10000.0
epsilon = 1e-06

def rotate(values, positions):
    half_dim = values.shape[-1] // 2
    inverse = jnp.power(jnp.float32(theta), -2.0 * jnp.arange(half_dim, dtype=jnp.float32) / values.shape[-1])
    angles = positions[:, None] * inverse[None, :]
    new_shape = (angles.shape[0],) + (1,) * (values.ndim - 2) + (half_dim,)
    cosine = jnp.cos(angles).reshape(new_shape)
    sine_part = jnp.sin(angles).reshape(new_shape)
    floats = values.astype(jnp.float32)
    lower_half = floats[..., :half_dim]
    upper_half = floats[..., half_dim:]
    turned = jnp.concatenate([lower_half * cosine - upper_half * sine_part, lower_half * sine_part + upper_half * cosine], axis=-1)
    return turned.astype(jnp.bfloat16)

def attend(query_turned, key_part, value_part, rope_turned, factor):
    nope_dim = key_part.shape[-1]
    head_count = query_turned.shape[1]
    block_rows = math.gcd(TOKENS, 512)
    grouped = query_turned.reshape(TOKENS // block_rows, block_rows, head_count, query_turned.shape[-1])
    key_float = key_part.astype(jnp.float32)
    rope_float = rope_turned.astype(jnp.float32)
    value_float = value_part.astype(jnp.float32)

    def one_block(query_block):
        query_float = query_block.astype(jnp.float32)
        scores = jnp.einsum('qhd,khd->hqk', query_float[..., :nope_dim], key_float)
        scores = (scores + jnp.einsum('qhd,kd->hqk', query_float[..., nope_dim:], rope_float)) * factor
        row_max = lax.optimization_barrier(jnp.max(scores, axis=-1, keepdims=True))
        weights = jnp.exp(scores - row_max)
        row_total = lax.optimization_barrier(jnp.sum(weights, axis=-1))
        rounded = lax.optimization_barrier(weights.astype(jnp.bfloat16)).astype(jnp.float32)
        weighted = jnp.einsum('hqk,khd->qhd', rounded, value_float)
        return (weighted / jnp.transpose(row_total)[:, :, None]).astype(jnp.bfloat16)
    outputs = lax.map(one_block, grouped)
    return outputs.reshape(TOKENS, head_count * value_part.shape[-1])

def turn_query(queries, head_count, nope_dim, positions):
    shaped = queries.reshape(TOKENS, head_count, nope_dim + ROPE)
    return jnp.concatenate([shaped[..., :nope_dim], rotate(shaped[..., nope_dim:], positions)], axis=-1)

def convolve(values, tap_rows):
    floats = values.astype(jnp.float32)
    zero_row = jnp.zeros((1, floats.shape[1]), jnp.float32)
    before = jnp.concatenate([zero_row, floats[:-1]], axis=0)
    after = jnp.concatenate([floats[1:], zero_row], axis=0)
    return tap_rows[0] * before + tap_rows[1] * floats + tap_rows[2] * after

def reference(residual, query_wide, query_narrow, latent, rope_key, latent_gain, expand_wide, expand_narrow, out_wide, out_narrow, norm_gain, up_gate, up_value, down_weight, conv_taps):
    positions = jnp.arange(TOKENS, dtype=jnp.int32).astype(jnp.float32)
    latent_float = latent.astype(jnp.float32)
    normed_latent = (latent_float * lax.rsqrt(lax.optimization_barrier(jnp.mean(latent_float * latent_float, axis=-1, keepdims=True)) + epsilon) * latent_gain).astype(jnp.bfloat16)
    rope_turned = rotate(rope_key, positions)
    kv_wide = jnp.dot(normed_latent, expand_wide, preferred_element_type=jnp.float32).astype(jnp.bfloat16).reshape(TOKENS, HW, NOPE_W + VAL_W)
    kv_narrow = jnp.dot(normed_latent, expand_narrow, preferred_element_type=jnp.float32).astype(jnp.bfloat16).reshape(TOKENS, HN, NOPE_N + VAL_N)
    query_w = turn_query(query_wide, HW, NOPE_W, positions)
    query_n = turn_query(query_narrow, HN, NOPE_N, positions)
    heads_wide = attend(query_w, kv_wide[..., :NOPE_W], kv_wide[..., NOPE_W:], rope_turned, (NOPE_W + ROPE) ** (-0.5))
    heads_narrow = attend(query_n, kv_narrow[..., :NOPE_N], kv_narrow[..., NOPE_N:], rope_turned, (NOPE_N + ROPE) ** (-0.5))
    wide_cols = HW // N_TP * VAL_W
    narrow_cols = HN // N_TP * VAL_N
    projected = jnp.zeros((TOKENS, D), jnp.float32)
    for group_index in range(N_TP):
        wide_slice = slice(group_index * wide_cols, (group_index + 1) * wide_cols)
        narrow_slice = slice(group_index * narrow_cols, (group_index + 1) * narrow_cols)
        partial_value = jnp.dot(heads_wide[:, wide_slice], out_wide[wide_slice], preferred_element_type=jnp.float32)
        partial_value = partial_value + jnp.dot(heads_narrow[:, narrow_slice], out_narrow[narrow_slice], preferred_element_type=jnp.float32)
        projected = projected + lax.optimization_barrier(partial_value.astype(jnp.bfloat16)).astype(jnp.float32)
    attended = (residual.astype(jnp.float32) + projected).astype(jnp.bfloat16)
    attended_float = attended.astype(jnp.float32)
    factor_rows = lax.rsqrt(lax.optimization_barrier(jnp.mean(attended_float * attended_float, axis=-1, keepdims=True)) + epsilon)
    normed = (attended_float * factor_rows * norm_gain).astype(jnp.bfloat16)
    gate_up = jnp.dot(normed, up_gate, preferred_element_type=jnp.float32).astype(jnp.bfloat16)
    value_up = jnp.dot(normed, up_value, preferred_element_type=jnp.float32).astype(jnp.bfloat16)
    hidden = (jax.nn.silu(convolve(gate_up, conv_taps[:, 0])) * convolve(value_up, conv_taps[:, 1])).astype(jnp.bfloat16)
    unit_cols = FF // N_TP
    channels = jnp.zeros((TOKENS, D), jnp.float32)
    for group_index in range(N_TP):
        unit_slice = slice(group_index * unit_cols, (group_index + 1) * unit_cols)
        partial_value = lax.dot_general(hidden[:, unit_slice], down_weight[:, unit_slice], (((1,), (1,)), ((), ())), preferred_element_type=jnp.float32)
        channels = channels + lax.optimization_barrier(partial_value.astype(jnp.bfloat16)).astype(jnp.float32)
    return (attended_float + channels).astype(jnp.bfloat16)
```

```python
import functools
import math

import jax
import jax.numpy as jnp
from jax import lax
from jax.experimental import pallas as pl
from jax.experimental.pallas import tpu as pltpu
from jax.sharding import PartitionSpec as P

D = 2048
ROPE = 64
NOPE_W = 128
VAL_W = 128
NOPE_N = 64
VAL_N = 64


theta = 10000.0
epsilon = 1e-06


def padded(block, sides, width):
    for axis, dim in sides:
        count = lax.axis_size(axis)
        forward = [(i, i + 1) for i in range(count - 1)]
        backward = [(target, source) for source, target in forward]
        low = lax.ppermute(
            lax.slice_in_dim(block, block.shape[dim] - width, None, axis=dim), axis, forward
        )
        high = lax.ppermute(lax.slice_in_dim(block, 0, width, axis=dim), axis, backward)
        block = jnp.concatenate([low, block, high], axis=dim)
    return block


def rotate(values, positions):
    half_dim = values.shape[-1] // 2
    inverse = jnp.power(
        jnp.float32(theta), -2.0 * jnp.arange(half_dim, dtype=jnp.float32) / values.shape[-1]
    )
    angles = positions[:, None] * inverse[None, :]
    new_shape = (angles.shape[0],) + (1,) * (values.ndim - 2) + (half_dim,)
    cosine = jnp.cos(angles).reshape(new_shape)
    sine_part = jnp.sin(angles).reshape(new_shape)
    floats = values.astype(jnp.float32)
    lower_half = floats[..., :half_dim]
    upper_half = floats[..., half_dim:]
    turned = jnp.concatenate(
        [
            lower_half * cosine - upper_half * sine_part,
            lower_half * sine_part + upper_half * cosine,
        ],
        axis=-1,
    )
    return turned.astype(jnp.bfloat16)


def turn_query(queries, head_count, nope_dim, positions):
    shaped = queries.reshape(queries.shape[0], head_count, nope_dim + ROPE)
    return jnp.concatenate(
        [shaped[..., :nope_dim], rotate(shaped[..., nope_dim:], positions)], axis=-1
    )


def attend_kernel(scale, chunk, q_ref, k_ref, v_ref, o_ref):
    query = q_ref[0]
    rows = query.shape[0]
    value_dim = v_ref.shape[-1]
    row_max = jnp.full((rows, 1), -1e30, jnp.float32)
    row_total = jnp.zeros((rows, 1), jnp.float32)
    weighted = jnp.zeros((rows, value_dim), jnp.float32)
    for start in range(0, k_ref.shape[1], chunk):
        scores = lax.dot_general(
            query,
            k_ref[0, start : start + chunk, :],
            (((1,), (1,)), ((), ())),
            preferred_element_type=jnp.float32,
        )
        new_max = jnp.maximum(row_max, jnp.max(scores, axis=-1, keepdims=True))
        weights = jnp.exp2((scores - new_max) * scale)
        keep = jnp.exp2((row_max - new_max) * scale)
        row_total = row_total * keep + jnp.sum(weights, axis=-1, keepdims=True)
        weighted = weighted * keep + jnp.dot(
            weights.astype(jnp.bfloat16),
            v_ref[0, start : start + chunk, :],
            preferred_element_type=jnp.float32,
        )
        row_max = new_max
    o_ref[0] = (weighted / row_total).astype(o_ref.dtype)


def attend(query, key, value, factor):
    heads, rows, width = query.shape
    count = key.shape[1]
    value_dim = value.shape[-1]
    block = math.gcd(rows, 320)
    chunk = math.gcd(count, 1024)
    return pl.pallas_call(
        functools.partial(attend_kernel, factor * math.log2(math.e), chunk),
        grid=(heads, rows // block),
        in_specs=[
            pl.BlockSpec((1, block, width), lambda h, i: (h, i, 0)),
            pl.BlockSpec((1, count, width), lambda h, i: (h, 0, 0)),
            pl.BlockSpec((1, count, value_dim), lambda h, i: (h, 0, 0)),
        ],
        out_specs=pl.BlockSpec((1, block, value_dim), lambda h, i: (h, i, 0)),
        out_shape=jax.ShapeDtypeStruct((heads, rows, value_dim), jnp.bfloat16),
        compiler_params=pltpu.CompilerParams(
            dimension_semantics=("arbitrary", "arbitrary"), vmem_limit_bytes=48 << 20
        ),
        cost_estimate=pl.CostEstimate(
            flops=2 * heads * rows * count * 512,
            bytes_accessed=2 * heads * count * (width + value_dim),
            transcendentals=heads * rows * count,
        ),
    )(query, key, value)


def key_value(latent, expand, head_count, key_dim, rope):
    pair = expand.reshape(expand.shape[0], head_count, -1)
    key = jnp.einsum(
        "td,dhn->htn", latent, pair[..., :key_dim], preferred_element_type=jnp.float32
    ).astype(jnp.bfloat16)
    value = jnp.einsum(
        "td,dhn->htn", latent, pair[..., key_dim:], preferred_element_type=jnp.float32
    ).astype(jnp.bfloat16)
    shared = jnp.broadcast_to(rope[None], (head_count,) + rope.shape)
    return jnp.concatenate([key, shared], axis=-1), value


def side_by_side(heads):
    return jnp.transpose(heads, (1, 0, 2)).reshape(heads.shape[1], -1)


def per_device(
    residual,
    query_wide,
    query_narrow,
    latent,
    rope_key,
    latent_gain,
    expand_wide,
    expand_narrow,
    out_wide,
    out_narrow,
    norm_gain,
    up_gate,
    up_value,
    down_weight,
    conv_taps,
):
    tok_rows = residual.shape[0]
    offset = lax.axis_index("sp") * tok_rows
    positions = (offset + lax.iota(jnp.int32, tok_rows)).astype(jnp.float32)
    latent_float = latent.astype(jnp.float32)
    normed_latent = (
        latent_float
        * lax.rsqrt(jnp.mean(latent_float * latent_float, axis=-1, keepdims=True) + epsilon)
        * latent_gain
    ).astype(jnp.bfloat16)
    rope_turned = rotate(rope_key, positions)
    wide_heads = query_wide.shape[1] // (NOPE_W + ROPE)
    narrow_heads = query_narrow.shape[1] // (NOPE_N + ROPE)
    query_w = turn_query(query_wide, wide_heads, NOPE_W, positions)
    query_n = turn_query(query_narrow, narrow_heads, NOPE_N, positions)
    gathered = lax.all_gather(
        jnp.concatenate([normed_latent, rope_turned, jnp.zeros_like(rope_turned)], axis=1),
        "sp",
        axis=0,
        tiled=True,
    )
    full_gain = lax.all_gather(norm_gain, "tp", axis=0, tiled=True)
    gathered, up_gate, up_value, down_weight = lax.optimization_barrier(
        (gathered, up_gate, up_value, down_weight)
    )
    gate_full, value_full, down_full = (
        lax.all_gather(up_gate, "sp", axis=0, tiled=True),
        lax.all_gather(up_value, "sp", axis=0, tiled=True),
        lax.all_gather(down_weight, "sp", axis=0, tiled=True),
    )
    rank = latent.shape[1]
    latent_all, rope_all = gathered[:, :rank], gathered[:, rank : rank + ROPE]
    key_w, value_w = key_value(latent_all, expand_wide, wide_heads, NOPE_W, rope_all)
    key_n, value_n = key_value(latent_all, expand_narrow, narrow_heads, NOPE_N, rope_all)
    heads_wide = side_by_side(
        attend(jnp.transpose(query_w, (1, 0, 2)), key_w, value_w, (NOPE_W + ROPE) ** (-0.5))
    )
    heads_narrow = side_by_side(
        attend(jnp.transpose(query_n, (1, 0, 2)), key_n, value_n, (NOPE_N + ROPE) ** (-0.5))
    )
    head_terms = jnp.dot(heads_wide, out_wide, preferred_element_type=jnp.float32)
    head_terms = head_terms + jnp.dot(heads_narrow, out_narrow, preferred_element_type=jnp.float32)
    head_terms, gate_full, value_full = lax.optimization_barrier(
        (head_terms.astype(jnp.bfloat16), gate_full, value_full)
    )
    head_shares = lax.psum_scatter(
        head_terms, "tp", scatter_dimension=1, tiled=True
    ).astype(jnp.float32)
    attended = (residual.astype(jnp.float32) + head_shares).astype(jnp.bfloat16)
    attended_float = attended.astype(jnp.float32)
    attended_full = lax.all_gather(attended, "tp", axis=1, tiled=True).astype(jnp.float32)
    squares = jnp.mean(attended_full * attended_full, axis=-1, keepdims=True)
    normed_full = (attended_full * lax.rsqrt(squares + epsilon) * full_gain).astype(jnp.bfloat16)
    gate_float = jnp.dot(normed_full, gate_full, preferred_element_type=jnp.float32)
    value_float = jnp.dot(normed_full, value_full, preferred_element_type=jnp.float32)
    gate_width = up_gate.shape[1]
    both_up = jnp.concatenate(
        [gate_float.astype(jnp.bfloat16), value_float.astype(jnp.bfloat16)], axis=1
    )
    extended = padded(both_up, (("sp", 0),), 1).astype(jnp.float32)
    tap_rows = conv_taps.reshape(3, 2 * gate_width)
    smoothed = (
        tap_rows[0] * extended[:-2] + tap_rows[1] * extended[1:-1] + tap_rows[2] * extended[2:]
    )
    hidden = (jax.nn.silu(smoothed[:, :gate_width]) * smoothed[:, gate_width:]).astype(jnp.bfloat16)
    unit_terms = lax.dot_general(
        hidden, down_full, (((1,), (1,)), ((), ())), preferred_element_type=jnp.float32
    )
    unit_shares = lax.psum_scatter(
        unit_terms.astype(jnp.bfloat16), "tp", scatter_dimension=1, tiled=True
    ).astype(jnp.float32)
    return (attended_float + unit_shares).astype(jnp.bfloat16)


def solution(mesh):
    in_specs = (
        P("sp", "tp"),
        P("sp", "tp"),
        P("sp", "tp"),
        P("sp", None),
        P("sp", None),
        P(),
        P(None, "tp"),
        P(None, "tp"),
        P("tp", None),
        P("tp", None),
        P("tp"),
        P("sp", "tp"),
        P("sp", "tp"),
        P("sp", "tp"),
        P(None, None, "tp"),
    )
    out_specs = P("sp", "tp")
    return jax.shard_map(
        per_device, mesh=mesh, in_specs=in_specs, out_specs=out_specs, check_vma=False
    )
```
